32 devices in a mesh: row: 8 (over z, core), col: 4 (over y, x).
Axes of the slice: x: 2, y: 2, z: 4, core: 2. Of those that a mesh axis runs over, the one named last changes fastest.
Arguments:
- tokens: bfloat16 [4096, 2048], P('row'), may hold values from -6 to 6
- out_weight: bfloat16 [2048, 2048], P(None, 'col'), may hold values from -0.125 to 0.125
Outputs:
- mixed: bfloat16 [4096, 2048], P('row', 'col')
The draws below stay inside these ranges and needn't reach their ends.
All inputs are finite; a program needn't handle non-finite values.
Results may differ from the reference program's by a relative error of at most 0.001.
Values may be sent and summed in bfloat16 or wider, within the bound.
No kernel may reach another device: no remote copies, remote signals or barrier semaphores. Data moves between devices by JAX's collectives and lax.ppermute only.
A program may use at most 64 MiB of HBM per device.

```python
import jax
import jax.numpy as jnp
from jax import lax

D = 2048
GROUPS = 4
GROUP_DIM = 512
LENGTH = 4096


def levels(own_key, extent, split, smallest, largest):
    def one(axis_at, parts):
        draws = jax.random.uniform(jax.random.fold_in(jax.random.fold_in(own_key, 6), axis_at), (parts,), jnp.float32, smallest / len(split), largest / len(split))
        return jnp.repeat(jnp.exp(draws), extent[axis_at] // parts).reshape((-1,) + (1,) * (len(extent) - axis_at - 1))

    factor_of = one(*split[0])
    for cut in split[1:]:
        factor_of = factor_of * one(*cut)
    return factor_of


def noise(rng, extent, width, bound, cuts=(), dtype=jnp.bfloat16):
    drawn = width * jax.random.normal(rng, extent, jnp.float32)
    if cuts:
        drawn = drawn * levels(rng, extent, cuts, -0.22, 0.18)
    return jnp.clip(drawn, -bound, bound).astype(dtype)


def setup_inputs(seed: int = 0) -> dict:
    keys = jax.random.split(jax.random.key(seed), 3)
    tokens = noise(keys[0], (LENGTH, D), 1.0, 6.0, ((0, 8),))
    out_weight = noise(keys[1], (D, D), D ** -0.5, 0.125, ((1, 4),))
    return {"tokens": tokens, "out_weight": out_weight}


def per_group(block):
    return jnp.fft.fft2(block, norm="ortho").real.astype(jnp.float32)


def reference(tokens, out_weight):
    grouped = tokens.astype(jnp.float32).reshape(LENGTH, GROUPS, GROUP_DIM)
    spectra = lax.map(per_group, jnp.moveaxis(grouped, 1, 0))
    spectral = jnp.moveaxis(spectra, 0, 1).reshape(LENGTH, D).astype(jnp.float32)
    mixed = jnp.dot(spectral, out_weight.astype(jnp.float32), precision=lax.Precision.HIGHEST, preferred_element_type=jnp.float32)
    return mixed.astype(jnp.bfloat16)
```

```python
import math

import jax
import jax.numpy as jnp
import numpy as np
from jax import lax
from jax.experimental import pallas as pl
from jax.experimental.pallas import tpu as pltpu
from jax.sharding import PartitionSpec as P

GROUPS = 4
GROUP_DIM = 512
HALF = GROUP_DIM // 2
BF = jnp.bfloat16
F32 = jnp.float32


def two_parts(table):
    high = np.asarray(table, np.float32).astype(BF)
    low = (np.asarray(table, np.float64) - high.astype(np.float64)).astype(np.float32).astype(BF)
    return high, low


def split(value):
    high = value.astype(BF)
    return high, (value - high.astype(F32)).astype(BF)


def dot_nt(left, right):
    return lax.dot_general(left, right, (((1,), (1,)), ((), ())), preferred_element_type=F32)


def dot_nn(left, right):
    return jnp.dot(left, right, preferred_element_type=F32)


def position_kernel(x_ref, m_ref, tw_c, tw_s, th_ref, tl_ref, o_ref, lh_ref, ll_ref):
    rows, chans, seg = x_ref.shape
    pairs = chans // 2
    cols = o_ref.shape[1]
    kb = o_ref.shape[2]
    mask = m_ref[...]
    evens, odds = [], []
    for r in range(rows):
        block = x_ref[r].astype(F32)
        lo, hi = block[:pairs], block[pairs:]
        evens.append(lo + mask * hi)
        odds.append(mask * lo + (1.0 - 2.0 * mask) * hi)

    def combine(values, j):
        real, imag = None, None
        for r in range(rows):
            c = math.cos(2 * math.pi * ((r * j) % rows) / rows)
            s = -math.sin(2 * math.pi * ((r * j) % rows) / rows)
            for kind, w in (("r", c), ("i", s)):
                if abs(w) < 1e-9:
                    continue
                if abs(abs(w) - 1.0) < 1e-9:
                    term = values[r] if w > 0 else -values[r]
                else:
                    term = w * values[r]
                if kind == "r":
                    real = term if real is None else real + term
                else:
                    imag = term if imag is None else imag + term
        if imag is None:
            imag = jnp.zeros_like(real)
        return real, imag

    def place(at, left, right):
        for side, value in ((0, left), (seg, right)):
            high, low = split(value)
            lh_ref[at : at + pairs, side : side + seg] = high
            ll_ref[at : at + pairs, side : side + seg] = low

    for j0 in range(rows // 2 + 1):
        er, ei = combine(evens, j0)
        orr, oi = combine(odds, j0)
        for j, sign in ((j0, 1.0), (rows - j0, -1.0)):
            if j == rows or (sign < 0 and j == j0):
                continue
            c, s = tw_c[j : j + 1], tw_s[j : j + 1]
            ein, oin = sign * ei, sign * oi
            place(j * chans, er * c + ein * s, ein * c - er * s)
            tr, ti = orr * c + oin * s, oin * c - orr * s
            place(
                j * chans + pairs,
                (1.0 - mask) * tr - mask * ti,
                mask * tr + (1.0 - mask) * ti,
            )
    width = o_ref.shape[3]
    for c in range(cols):
        lh, ll = lh_ref[c * width : (c + 1) * width], ll_ref[c * width : (c + 1) * width]
        th = th_ref[...]
        z = dot_nt(th, lh) + dot_nt(th, ll) + dot_nt(tl_ref[...], lh)
        for r in range(rows):
            o_ref[r, c] = z[r * kb : (r + 1) * kb]


def output_kernel(at_ref, z_ref, gh_ref, gl_ref, mine_ref, other_ref, o_ref, zh_ref, zl_ref, sh_ref, sl_ref):
    rows, cols, kb, width = z_ref.shape
    step = pl.program_id(0)
    total = zh_ref.shape[1]
    chans = total // (rows * cols)
    jb = width // chans

    @pl.when(step == 0)
    def _():
        for c in range(cols):
            for r in range(rows):
                block = z_ref[r, c]
                high, low = split(block)
                lane = (c * rows + r) * chans
                for jj in range(jb):
                    zh_ref[jj * kb : (jj + 1) * kb, lane : lane + chans] = high[:, jj * chans : (jj + 1) * chans]
                    zl_ref[jj * kb : (jj + 1) * kb, lane : lane + chans] = low[:, jj * chans : (jj + 1) * chans]
        for g in range(GROUPS):
            cut = slice(g * GROUP_DIM, (g + 1) * GROUP_DIM)
            zh, zl = zh_ref[:, cut], zl_ref[:, cut]
            gh = gh_ref[...]
            spectral = dot_nn(zh, gh) + dot_nn(zl, gh) + dot_nn(zh, gl_ref[...])
            high, low = split(spectral)
            half, at = divmod(g * GROUP_DIM, total // 2)
            sh_ref[half, :, at : at + GROUP_DIM] = high
            sl_ref[half, :, at : at + GROUP_DIM] = low

    half = at_ref[0]
    mine, other = mine_ref[0], other_ref[0]
    result = dot_nn(sh_ref[half], mine) + dot_nn(sl_ref[half], mine)
    result = result + dot_nn(sh_ref[1 - half], other) + dot_nn(sl_ref[1 - half], other)
    o_ref[0] = result.astype(BF)


def body(tokens, out_weight):
    seg, dim = tokens.shape
    out_cols = out_weight.shape[1]
    rows = lax.axis_size("row")
    cols = lax.axis_size("col")
    row, col = lax.axis_index("row"), lax.axis_index("col")
    length = seg * rows
    chans = dim // (rows * cols)
    pairs = chans // 2
    jb, kb = rows // cols, seg // rows

    half = row % 2
    own = lax.dynamic_slice(out_weight, (half * (dim // 2), 0), (dim // 2, out_cols))
    rest = lax.dynamic_slice(out_weight, ((1 - half) * (dim // 2), 0), (dim // 2, out_cols))
    fetched = [
        lax.ppermute(own, "col", [(c, c ^ d) for c in range(cols)]) for d in range(1, cols)
    ]
    mine = jnp.stack([own] + fetched)
    swapped = [lax.ppermute(f, "row", [(r, r ^ 1) for r in range(rows)]) for f in fetched]
    other = jnp.stack([rest] + swapped)

    group = (col * GROUPS) // cols
    group_tokens = lax.dynamic_slice(tokens, (0, group * GROUP_DIM), (seg, GROUP_DIM))
    slot = jnp.arange(rows * chans, dtype=jnp.int32)
    pair = (col * rows + slot // chans) * pairs + (slot % chans) % pairs
    p = pair % HALF
    upper = (slot % chans) >= pairs
    channel = jnp.where(upper, jnp.where(p == 0, HALF, GROUP_DIM - p), p)
    pick = (channel[:, None] == jnp.arange(GROUP_DIM, dtype=jnp.int32)[None, :]).astype(BF)
    turned = dot_nt(pick, group_tokens).astype(BF).reshape(rows, chans, seg)
    whole = lax.all_to_all(turned, "row", split_axis=0, concat_axis=0, tiled=True)

    own_pair = (col * rows + row) * pairs + jnp.arange(pairs, dtype=jnp.int32)
    mask = ((own_pair % HALF) != 0).astype(F32)[:, None]
    s_at = np.arange(seg)
    twist = 2 * np.pi * ((np.arange(rows)[:, None] * s_at[None, :]) % length) / length
    phase = 2 * np.pi * ((s_at[:, None] * s_at[None, :]) % seg) / seg
    th, tl = two_parts(np.concatenate([np.cos(phase), np.sin(phase)], axis=1))
    spread = pl.pallas_call(
        position_kernel,
        out_shape=jax.ShapeDtypeStruct((rows, cols, kb, jb * chans), F32),
        scratch_shapes=[pltpu.VMEM((rows * chans, 2 * seg), BF)] * 2,
        name="positions",
    )(whole, mask, np.cos(twist).astype(np.float32), np.sin(twist).astype(np.float32), th, tl)
    flat = spread.reshape(rows * cols, kb, jb * chans)
    mixed_in = lax.all_to_all(flat, ("row", "col"), split_axis=0, concat_axis=0, tiled=True)
    mixed_in = mixed_in.reshape(rows, cols, kb, jb * chans)

    lanes = np.arange(GROUP_DIM)
    lp = (lanes // chans) * pairs + (lanes % chans) % pairs
    odd = (lanes % chans) >= pairs
    turn = 2 * np.pi * ((lp[:, None] * lanes[None, :]) % GROUP_DIM) / GROUP_DIM
    flip = np.where(lanes % 2 == 0, 1.0, -1.0)[None, :]
    grid_table = np.where(odd[:, None], np.where(lp[:, None] == 0, flip, -np.sin(turn)), np.cos(turn))
    gh, gl = two_parts(grid_table / math.sqrt(length * GROUP_DIM))
    places = jnp.stack([half, col]).astype(jnp.int32)
    few = jb * kb
    whole_spec = lambda shape: pl.BlockSpec(shape, lambda d, at: (0,) * len(shape))
    out = pl.pallas_call(
        output_kernel,
        out_shape=jax.ShapeDtypeStruct((cols, few, out_cols), BF),
        grid_spec=pltpu.PrefetchScalarGridSpec(
            num_scalar_prefetch=1,
            grid=(cols,),
            in_specs=[
                whole_spec(mixed_in.shape),
                whole_spec((GROUP_DIM, GROUP_DIM)),
                whole_spec((GROUP_DIM, GROUP_DIM)),
                pl.BlockSpec((1, dim // 2, out_cols), lambda d, at: (d, 0, 0)),
                pl.BlockSpec((1, dim // 2, out_cols), lambda d, at: (d, 0, 0)),
            ],
            out_specs=pl.BlockSpec((1, few, out_cols), lambda d, at: (jnp.bitwise_xor(d, at[1]), 0, 0)),
            scratch_shapes=[pltpu.VMEM((few, dim), BF)] * 2 + [pltpu.VMEM((2, few, dim // 2), BF)] * 2,
        ),
        name="outputs",
    )(places, mixed_in, gh, gl, mine, other)
    gathered = lax.all_to_all(out, "col", split_axis=0, concat_axis=0, tiled=True)
    gathered = gathered.reshape(seg, out_cols)
    at = jnp.arange(seg, dtype=jnp.int32)
    wanted = (at % rows) * kb + at // rows
    order = (wanted[:, None] == at[None, :]).astype(BF)
    return dot_nn(order, gathered).astype(BF)


def solution(mesh):
    placed = (P("row", None), P(None, "col"))
    return jax.shard_map(
        body, mesh=mesh, in_specs=placed, out_specs=P("row", "col"), check_vma=False
    )
```

```python
import math

import jax
import jax.numpy as jnp
import numpy as np
from jax import lax
from jax.experimental import pallas as pl
from jax.experimental.pallas import tpu as pltpu
from jax.sharding import PartitionSpec as P


GROUPS = 4
GROUP_DIM = 512
HALF = GROUP_DIM // 2
BF = jnp.bfloat16
F32 = jnp.float32


def two_parts(table):
    high = np.asarray(table, np.float32).astype(BF)
    low = (np.asarray(table, np.float64) - high.astype(np.float64)).astype(np.float32).astype(BF)
    return high, low


def split(value):
    high = value.astype(BF)
    return high, (value - high.astype(F32)).astype(BF)


def dot_nt(left, right):
    return lax.dot_general(left, right, (((1,), (1,)), ((), ())), preferred_element_type=F32)


def dot_nn(left, right):
    return jnp.dot(left, right, preferred_element_type=F32)


def plus(left, right, sign=1):
    if right is None:
        return left
    if left is None:
        return right if sign > 0 else -right
    return left + right if sign > 0 else left - right


def times(weight, value):
    if value is None or abs(weight) < 1e-9:
        return None
    if abs(weight - 1.0) < 1e-9:
        return value
    return -value if abs(weight + 1.0) < 1e-9 else weight * value


def real_dft(values):
    n = len(values)
    if n == 1:
        return [(values[0], None)]
    even, odd = real_dft(values[::2]), real_dft(values[1::2])
    terms = [None] * (n // 2 + 1)
    for k in range(n // 4 + 1):
        c, s = math.cos(2 * math.pi * k / n), -math.sin(2 * math.pi * k / n)
        re = plus(times(c, odd[k][0]), times(s, odd[k][1]), -1)
        im = plus(times(c, odd[k][1]), times(s, odd[k][0]))
        terms[n // 2 - k] = (plus(even[k][0], re, -1), times(-1.0, plus(even[k][1], im, -1)))
        terms[k] = (plus(even[k][0], re), plus(even[k][1], im))
    return terms


def position_kernel(x_ref, m_ref, tw_c, tw_s, th_ref, tl_ref, o_ref, lh_ref, ll_ref):
    rows, chans, seg = x_ref.shape
    pairs = chans // 2
    cols = o_ref.shape[1]
    kb = o_ref.shape[2]
    mask = m_ref[...]
    evens, odds = [], []
    for r in range(rows):
        block = x_ref[r].astype(F32)
        lo, hi = block[:pairs], block[pairs:]
        evens.append(lo + mask * hi)
        odds.append(mask * lo + (1.0 - 2.0 * mask) * hi)

    def place(at, left, right):
        for side, value in ((0, left), (seg, right)):
            high, low = split(value)
            lh_ref[at : at + pairs, side : side + seg] = high
            ll_ref[at : at + pairs, side : side + seg] = low

    zero = jnp.zeros((pairs, seg), F32)
    even_terms, odd_terms = real_dft(evens), real_dft(odds)
    for j0 in range(rows // 2 + 1):
        er, ei = (zero if v is None else v for v in even_terms[j0])
        orr, oi = (zero if v is None else v for v in odd_terms[j0])
        for j, sign in ((j0, 1.0), (rows - j0, -1.0)):
            if j == rows or (sign < 0 and j == j0):
                continue
            c, s = tw_c[j : j + 1], tw_s[j : j + 1]
            ein, oin = sign * ei, sign * oi
            place(j * chans, er * c + ein * s, ein * c - er * s)
            tr, ti = orr * c + oin * s, oin * c - orr * s
            place(
                j * chans + pairs,
                (1.0 - mask) * tr - mask * ti,
                mask * tr + (1.0 - mask) * ti,
            )
    width = o_ref.shape[3]
    for c in range(cols):
        lh, ll = lh_ref[c * width : (c + 1) * width], ll_ref[c * width : (c + 1) * width]
        th = th_ref[...]
        z = dot_nt(th, lh) + dot_nt(th, ll) + dot_nt(tl_ref[...], lh)
        for r in range(rows):
            o_ref[r, c] = z[r * kb : (r + 1) * kb]


def output_kernel(at_ref, z_ref, gh_ref, gl_ref, own_ref, *refs):
    rows, cols, kb, width = z_ref.shape
    total = own_ref.shape[0]
    mine, other = refs[: cols - 1], refs[cols - 1 : 2 * (cols - 1)]
    o_ref, zh_ref, zl_ref, sh_ref, own_v, mine_v, other_v, sems = refs[2 * (cols - 1) :]
    chans = total // (rows * cols)
    jb = width // chans
    own_copy = pltpu.make_async_copy(own_ref, own_v, sems.at[0])
    own_copy.start()
    copies = []
    for d in range(cols - 1):
        pair = (
            pltpu.make_async_copy(mine[d], mine_v.at[d], sems.at[1 + 2 * d]),
            pltpu.make_async_copy(other[d], other_v.at[d], sems.at[2 + 2 * d]),
        )
        for copy in pair:
            copy.start()
        copies.append(pair)

    for c in range(cols):
        for r in range(rows):
            high, low = split(z_ref[r, c])
            lane = (c * rows + r) * chans
            for jj in range(jb):
                zh_ref[jj * kb : (jj + 1) * kb, lane : lane + chans] = high[:, jj * chans : (jj + 1) * chans]
                zl_ref[jj * kb : (jj + 1) * kb, lane : lane + chans] = low[:, jj * chans : (jj + 1) * chans]
    few = jb * kb
    for g in range(GROUPS):
        cut = slice(g * GROUP_DIM, (g + 1) * GROUP_DIM)
        zh, zl = zh_ref[:, cut], zl_ref[:, cut]
        gh = gh_ref[...]
        spectral = dot_nn(zh, gh) + dot_nn(zl, gh) + dot_nn(zh, gl_ref[...])
        high, low = split(spectral)
        half, at = divmod(g * GROUP_DIM, total // 2)
        sh_ref[half, :few, at : at + GROUP_DIM] = high
        sh_ref[half, few:, at : at + GROUP_DIM] = low

    half, col = at_ref[0], at_ref[1]
    own_copy.wait()
    both = dot_nn(sh_ref[0], own_v[: total // 2]) + dot_nn(sh_ref[1], own_v[total // 2 :])
    o_ref[col] = (both[:few] + both[few:]).astype(BF)
    for d in range(cols - 1):
        for copy in copies[d]:
            copy.wait()
        both = dot_nn(sh_ref[half], mine_v[d]) + dot_nn(sh_ref[1 - half], other_v[d])
        o_ref[jnp.bitwise_xor(col, d + 1)] = (both[:few] + both[few:]).astype(BF)


def body(tokens, out_weight):
    seg, dim = tokens.shape
    out_cols = out_weight.shape[1]
    rows = lax.axis_size("row")
    cols = lax.axis_size("col")
    row, col = lax.axis_index("row"), lax.axis_index("col")
    length = seg * rows
    chans = dim // (rows * cols)
    pairs = chans // 2
    jb, kb = rows // cols, seg // rows

    half = row % 2
    own = lax.dynamic_slice(out_weight, (half * (dim // 2), 0), (dim // 2, out_cols))
    fetched, swapped = [], []
    for d in range(1, cols):
        fetched.append(lax.ppermute(own, "col", [(c, c ^ d) for c in range(cols)]))
        swapped.append(lax.ppermute(fetched[-1], "row", [(r, r ^ 1) for r in range(rows)]))

    group = (col * GROUPS) // cols
    group_tokens = lax.dynamic_slice(tokens, (0, group * GROUP_DIM), (seg, GROUP_DIM))
    slot = jnp.arange(rows * chans, dtype=jnp.int32)
    pair = (col * rows + slot // chans) * pairs + (slot % chans) % pairs
    p = pair % HALF
    upper = (slot % chans) >= pairs
    channel = jnp.where(upper, jnp.where(p == 0, HALF, GROUP_DIM - p), p)
    pick = (channel[:, None] == jnp.arange(GROUP_DIM, dtype=jnp.int32)[None, :]).astype(BF)
    turned = dot_nt(pick, group_tokens).astype(BF).reshape(rows, chans, seg)
    whole = lax.all_to_all(turned, "row", split_axis=0, concat_axis=0, tiled=True)

    own_pair = (col * rows + row) * pairs + jnp.arange(pairs, dtype=jnp.int32)
    mask = ((own_pair % HALF) != 0).astype(F32)[:, None]
    s_at = np.arange(seg)
    twist = 2 * np.pi * ((np.arange(rows)[:, None] * s_at[None, :]) % length) / length
    phase = 2 * np.pi * ((s_at[:, None] * s_at[None, :]) % seg) / seg
    th, tl = two_parts(np.concatenate([np.cos(phase), np.sin(phase)], axis=1))
    in_vmem = pl.BlockSpec(memory_space=pltpu.VMEM)
    spread = pl.pallas_call(
        position_kernel,
        out_shape=jax.ShapeDtypeStruct((rows, cols, kb, jb * chans), F32),
        in_specs=[in_vmem] * 6,
        scratch_shapes=[pltpu.VMEM((rows * chans, 2 * seg), BF)] * 2,
        compiler_params=pltpu.CompilerParams(vmem_limit_bytes=20 * 1024 * 1024),
        name="positions",
    )(whole, mask, np.cos(twist).astype(np.float32), np.sin(twist).astype(np.float32), th, tl)
    flat = spread.reshape(rows * cols, kb, jb * chans)
    mixed_in = lax.all_to_all(flat, ("row", "col"), split_axis=0, concat_axis=0, tiled=True)
    mixed_in = mixed_in.reshape(rows, cols, kb, jb * chans)

    lanes = np.arange(GROUP_DIM)
    lp = (lanes // chans) * pairs + (lanes % chans) % pairs
    odd = (lanes % chans) >= pairs
    turn = 2 * np.pi * ((lp[:, None] * lanes[None, :]) % GROUP_DIM) / GROUP_DIM
    flip = np.where(lanes % 2 == 0, 1.0, -1.0)[None, :]
    grid_table = np.where(odd[:, None], np.where(lp[:, None] == 0, flip, -np.sin(turn)), np.cos(turn))
    gh, gl = two_parts(grid_table / math.sqrt(length * GROUP_DIM))
    places = jnp.stack([half, col]).astype(jnp.int32)
    few = jb * kb
    anywhere = pl.BlockSpec(memory_space=pl.ANY)
    out = pl.pallas_call(
        output_kernel,
        out_shape=jax.ShapeDtypeStruct((cols, few, out_cols), BF),
        in_specs=[pl.BlockSpec(memory_space=pltpu.SMEM), in_vmem, in_vmem, in_vmem]
        + [anywhere] * (2 * cols - 1),
        scratch_shapes=[pltpu.VMEM((few, dim), BF)] * 2
        + [
            pltpu.VMEM((2, 2 * few, dim // 2), BF),
            pltpu.VMEM((dim, out_cols), BF),
            pltpu.VMEM((cols - 1, dim // 2, out_cols), BF),
            pltpu.VMEM((cols - 1, dim // 2, out_cols), BF),
            pltpu.SemaphoreType.DMA((2 * cols - 1,)),
        ],
        compiler_params=pltpu.CompilerParams(vmem_limit_bytes=26 * 1024 * 1024),
        name="outputs",
    )(places, mixed_in, gh, gl, out_weight, *fetched, *swapped)
    gathered = lax.all_to_all(out, "col", split_axis=0, concat_axis=0, tiled=True)
    gathered = gathered.reshape(seg, out_cols)
    at = jnp.arange(seg, dtype=jnp.int32)
    wanted = (at % rows) * kb + at // rows
    order = (wanted[:, None] == at[None, :]).astype(BF)
    return dot_nn(order, gathered).astype(BF)


def solution(mesh):
    placed = (P("row", None), P(None, "col"))
    return jax.shard_map(
        body, mesh=mesh, in_specs=placed, out_specs=P("row", "col"), check_vma=False
    )
```

```python
import math

import jax
import jax.numpy as jnp
import numpy as np
from jax import lax
from jax.experimental import pallas as pl
from jax.experimental.pallas import tpu as pltpu
from jax.sharding import PartitionSpec as P


GROUPS = 4
GROUP_DIM = 512
HALF = GROUP_DIM // 2
BF = jnp.bfloat16
F32 = jnp.float32


def two_parts(table):
    high = np.asarray(table, np.float32).astype(BF)
    low = (np.asarray(table, np.float64) - high.astype(np.float64)).astype(np.float32).astype(BF)
    return high, low


def split(value):
    high = value.astype(BF)
    return high, (value - high.astype(F32)).astype(BF)


def dot_nt(left, right):
    return lax.dot_general(left, right, (((1,), (1,)), ((), ())), preferred_element_type=F32)


def dot_nn(left, right):
    return jnp.dot(left, right, preferred_element_type=F32)


def plus(left, right, sign=1):
    if right is None:
        return left
    if left is None:
        return right if sign > 0 else -right
    return left + right if sign > 0 else left - right


def times(weight, value):
    if value is None or abs(weight) < 1e-9:
        return None
    if abs(weight - 1.0) < 1e-9:
        return value
    return -value if abs(weight + 1.0) < 1e-9 else weight * value


def real_dft(values):
    n = len(values)
    if n == 1:
        return [(values[0], None)]
    even, odd = real_dft(values[::2]), real_dft(values[1::2])
    terms = [None] * (n // 2 + 1)
    for k in range(n // 4 + 1):
        c, s = math.cos(2 * math.pi * k / n), -math.sin(2 * math.pi * k / n)
        re = plus(times(c, odd[k][0]), times(s, odd[k][1]), -1)
        im = plus(times(c, odd[k][1]), times(s, odd[k][0]))
        terms[n // 2 - k] = (plus(even[k][0], re, -1), times(-1.0, plus(even[k][1], im, -1)))
        terms[k] = (plus(even[k][0], re), plus(even[k][1], im))
    return terms


def position_kernel(x_ref, m_ref, tw_c, tw_s, th_in, tl_in, o_ref, lh_ref, ll_ref, th_ref, tl_ref, sems):
    rows, chans, seg = x_ref.shape
    pairs = chans // 2
    cols = o_ref.shape[1]
    kb = o_ref.shape[2]
    tables = (
        pltpu.make_async_copy(th_in, th_ref, sems.at[0]),
        pltpu.make_async_copy(tl_in, tl_ref, sems.at[1]),
    )
    for copy in tables:
        copy.start()
    mask = m_ref[...]
    evens, odds = [], []
    for r in range(rows):
        block = x_ref[r].astype(F32)
        lo, hi = block[:pairs], block[pairs:]
        evens.append(lo + mask * hi)
        odds.append(mask * lo + (1.0 - 2.0 * mask) * hi)

    def place(at, left, right):
        for side, value in ((0, left), (seg, right)):
            high, low = split(value)
            lh_ref[at : at + pairs, side : side + seg] = high
            ll_ref[at : at + pairs, side : side + seg] = low

    zero = jnp.zeros((pairs, seg), F32)
    even_terms, odd_terms = real_dft(evens), real_dft(odds)
    for j0 in range(rows // 2 + 1):
        er, ei = (zero if v is None else v for v in even_terms[j0])
        orr, oi = (zero if v is None else v for v in odd_terms[j0])
        for j, sign in ((j0, 1.0), (rows - j0, -1.0)):
            if j == rows or (sign < 0 and j == j0):
                continue
            c, s = tw_c[j : j + 1], tw_s[j : j + 1]
            ein, oin = sign * ei, sign * oi
            place(j * chans, er * c + ein * s, ein * c - er * s)
            tr, ti = orr * c + oin * s, oin * c - orr * s
            place(
                j * chans + pairs,
                (1.0 - mask) * tr - mask * ti,
                mask * tr + (1.0 - mask) * ti,
            )
    width = o_ref.shape[3]
    for copy in tables:
        copy.wait()
    for c in range(cols):
        lh, ll = lh_ref[c * width : (c + 1) * width], ll_ref[c * width : (c + 1) * width]
        th = th_ref[...]
        z = dot_nt(th, lh) + dot_nt(th, ll) + dot_nt(tl_ref[...], lh)
        for r in range(rows):
            o_ref[r, c] = z[r * kb : (r + 1) * kb]


def output_kernel(at_ref, z_ref, gh_in, gl_in, own_ref, *refs):
    rows, cols, kb, width = z_ref.shape
    total = own_ref.shape[0]
    mine, other = refs[: cols - 1], refs[cols - 1 : 2 * (cols - 1)]
    o_ref, zh_ref, zl_ref, sh_ref, own_v, mine_v, other_v, gh_ref, gl_ref, sems = refs[2 * (cols - 1) :]
    chans = total // (rows * cols)
    jb = width // chans
    tables = (
        pltpu.make_async_copy(gh_in, gh_ref, sems.at[2 * cols - 1]),
        pltpu.make_async_copy(gl_in, gl_ref, sems.at[2 * cols]),
    )
    for copy in tables:
        copy.start()
    own_copy = pltpu.make_async_copy(own_ref, own_v, sems.at[0])
    own_copy.start()
    copies = []
    for d in range(cols - 1):
        pair = (
            pltpu.make_async_copy(mine[d], mine_v.at[d], sems.at[1 + 2 * d]),
            pltpu.make_async_copy(other[d], other_v.at[d], sems.at[2 + 2 * d]),
        )
        for copy in pair:
            copy.start()
        copies.append(pair)

    for c in range(cols):
        for r in range(rows):
            high, low = split(z_ref[r, c])
            lane = (c * rows + r) * chans
            for jj in range(jb):
                zh_ref[jj * kb : (jj + 1) * kb, lane : lane + chans] = high[:, jj * chans : (jj + 1) * chans]
                zl_ref[jj * kb : (jj + 1) * kb, lane : lane + chans] = low[:, jj * chans : (jj + 1) * chans]
    few = jb * kb
    for copy in tables:
        copy.wait()
    for g in range(GROUPS):
        cut = slice(g * GROUP_DIM, (g + 1) * GROUP_DIM)
        zh, zl = zh_ref[:, cut], zl_ref[:, cut]
        gh = gh_ref[...]
        spectral = dot_nn(zh, gh) + dot_nn(zl, gh) + dot_nn(zh, gl_ref[...])
        high, low = split(spectral)
        half, at = divmod(g * GROUP_DIM, total // 2)
        sh_ref[half, :few, at : at + GROUP_DIM] = high
        sh_ref[half, few:, at : at + GROUP_DIM] = low

    half, col = at_ref[0], at_ref[1]
    own_copy.wait()
    both = dot_nn(sh_ref[0], own_v[: total // 2]) + dot_nn(sh_ref[1], own_v[total // 2 :])
    o_ref[col] = (both[:few] + both[few:]).astype(BF)
    for d in range(cols - 1):
        for copy in copies[d]:
            copy.wait()
        both = dot_nn(sh_ref[half], mine_v[d]) + dot_nn(sh_ref[1 - half], other_v[d])
        o_ref[jnp.bitwise_xor(col, d + 1)] = (both[:few] + both[few:]).astype(BF)


def body(tokens, out_weight):
    seg, dim = tokens.shape
    out_cols = out_weight.shape[1]
    rows = lax.axis_size("row")
    cols = lax.axis_size("col")
    row, col = lax.axis_index("row"), lax.axis_index("col")
    length = seg * rows
    chans = dim // (rows * cols)
    pairs = chans // 2
    jb, kb = rows // cols, seg // rows

    half = row % 2
    own = lax.dynamic_slice(out_weight, (half * (dim // 2), 0), (dim // 2, out_cols))
    fetched, swapped = [], []
    for d in range(1, cols):
        fetched.append(lax.ppermute(own, "col", [(c, c ^ d) for c in range(cols)]))
        swapped.append(lax.ppermute(fetched[-1], "row", [(r, r ^ 1) for r in range(rows)]))

    group = (col * GROUPS) // cols
    group_tokens = lax.dynamic_slice(tokens, (0, group * GROUP_DIM), (seg, GROUP_DIM))
    slot = jnp.arange(rows * chans, dtype=jnp.int32)
    pair = (col * rows + slot // chans) * pairs + (slot % chans) % pairs
    p = pair % HALF
    upper = (slot % chans) >= pairs
    channel = jnp.where(upper, jnp.where(p == 0, HALF, GROUP_DIM - p), p)
    pick = (channel[:, None] == jnp.arange(GROUP_DIM, dtype=jnp.int32)[None, :]).astype(BF)
    turned = dot_nt(pick, group_tokens).astype(BF).reshape(rows, chans, seg)
    whole = lax.all_to_all(turned, "row", split_axis=0, concat_axis=0, tiled=True)

    own_pair = (col * rows + row) * pairs + jnp.arange(pairs, dtype=jnp.int32)
    mask = ((own_pair % HALF) != 0).astype(F32)[:, None]
    s_at = np.arange(seg)
    twist = 2 * np.pi * ((np.arange(rows)[:, None] * s_at[None, :]) % length) / length
    phase = 2 * np.pi * ((s_at[:, None] * s_at[None, :]) % seg) / seg
    th, tl = two_parts(np.concatenate([np.cos(phase), np.sin(phase)], axis=1))
    in_vmem = pl.BlockSpec(memory_space=pltpu.VMEM)
    in_hbm = pl.BlockSpec(memory_space=pltpu.HBM)
    spread = pl.pallas_call(
        position_kernel,
        out_shape=jax.ShapeDtypeStruct((rows, cols, kb, jb * chans), F32),
        in_specs=[in_vmem] * 4 + [in_hbm] * 2,
        scratch_shapes=[pltpu.VMEM((rows * chans, 2 * seg), BF)] * 2
        + [pltpu.VMEM((seg, 2 * seg), BF)] * 2
        + [pltpu.SemaphoreType.DMA((2,))],
        name="positions",
    )(whole, mask, np.cos(twist).astype(np.float32), np.sin(twist).astype(np.float32), th, tl)
    flat = spread.reshape(rows * cols, kb, jb * chans)
    mixed_in = lax.all_to_all(flat, ("row", "col"), split_axis=0, concat_axis=0, tiled=True)
    mixed_in = mixed_in.reshape(rows, cols, kb, jb * chans)

    lanes = np.arange(GROUP_DIM)
    lp = (lanes // chans) * pairs + (lanes % chans) % pairs
    odd = (lanes % chans) >= pairs
    turn = 2 * np.pi * ((lp[:, None] * lanes[None, :]) % GROUP_DIM) / GROUP_DIM
    flip = np.where(lanes % 2 == 0, 1.0, -1.0)[None, :]
    grid_table = np.where(odd[:, None], np.where(lp[:, None] == 0, flip, -np.sin(turn)), np.cos(turn))
    gh, gl = two_parts(grid_table / math.sqrt(length * GROUP_DIM))
    places = jnp.stack([half, col]).astype(jnp.int32)
    few = jb * kb
    out = pl.pallas_call(
        output_kernel,
        out_shape=jax.ShapeDtypeStruct((cols, few, out_cols), BF),
        in_specs=[pl.BlockSpec(memory_space=pltpu.SMEM), in_vmem]
        + [in_hbm] * (2 * cols + 1),
        scratch_shapes=[pltpu.VMEM((few, dim), BF)] * 2
        + [
            pltpu.VMEM((2, 2 * few, dim // 2), BF),
            pltpu.VMEM((dim, out_cols), BF),
            pltpu.VMEM((cols - 1, dim // 2, out_cols), BF),
            pltpu.VMEM((cols - 1, dim // 2, out_cols), BF),
            pltpu.VMEM((GROUP_DIM, GROUP_DIM), BF),
            pltpu.VMEM((GROUP_DIM, GROUP_DIM), BF),
            pltpu.SemaphoreType.DMA((2 * cols + 1,)),
        ],
        name="outputs",
    )(places, mixed_in, gh, gl, out_weight, *fetched, *swapped)
    gathered = lax.all_to_all(out, "col", split_axis=0, concat_axis=0, tiled=True)
    gathered = gathered.reshape(seg, out_cols)
    at = jnp.arange(seg, dtype=jnp.int32)
    wanted = (at % rows) * kb + at // rows
    order = (wanted[:, None] == at[None, :]).astype(BF)
    return dot_nn(order, gathered).astype(BF)


def solution(mesh):
    placed = (P("row", None), P(None, "col"))
    return jax.shard_map(
        body, mesh=mesh, in_specs=placed, out_specs=P("row", "col"), check_vma=False
    )
```
